32 devices in a mesh: sp: 4 (over x, core), tp: 8 (over z, y).
Axes of the slice: x: 2, y: 2, z: 4, core: 2. Of those that a mesh axis runs over, the one named last changes fastest.
Arguments:
- tokens: bfloat16 [4, 1024, 2048], P(None, ('sp', 'tp')), may hold values from -6 to 6
- norm_gain: float32 [2048], replicated, may hold values from 0.5 to 1.5
- entry_projection: bfloat16 [2048, 2048], P(None, 'tp'), may hold values from -0.125 to 0.125
- valve_projection: bfloat16 [2048, 2048], P(None, 'tp'), may hold values from -0.125 to 0.125
- filter_taps: float32 [4, 2048], P(None, 'tp'), may hold values from -3 to 3
- conv_bias: float32 [2048], P('tp'), may hold values from -0.6 to 0.6
- recur_weight: bfloat16 [16, 128, 128], P('tp'), may hold values from -0.5 to 0.5
- recur_bias: float32 [2048], P('tp'), may hold values from -3 to 3
- entry_weight: bfloat16 [16, 128, 128], P('tp'), may hold values from -0.5 to 0.5
- entry_bias: float32 [2048], P('tp'), may hold values from -0.6 to 0.6
- forget_rate: float32 [2048], P('tp'), may hold values from 6.1035156e-05 to 0.25, as said below
- output_weight: bfloat16 [2048, 2048], P('tp'), may hold values from -0.5 to 0.5
Outputs:
- mixed: bfloat16 [4, 1024, 2048], P(None, ('sp', 'tp'))
The draws below stay inside these ranges and needn't reach their ends.
Inputs may be any that keep to these rules, and one draw needn't show every extreme that they name: forget_rate is positive; its even channels lie between 1 / 16384 and 1 / 4096, its odd channels between 1 / 64 and 1 / 4.
All inputs are finite; a program needn't handle non-finite values.
Results may differ from the reference program's by a relative error of at most 0.02.
Values may be sent and summed in bfloat16 or wider, within the bound.
A program may use at most 64 MiB of HBM per device.

```python
import jax
import jax.numpy as jnp
from jax import lax

D = 2048
D_LRU = 2048
BLOCKS = 16
WIDTH_BLOCK = 128
CONV_W = 4
SEQS = 4
SEQ_LEN = 1024


def draw_forget_rate(key, part):
    minimum_decay_bound = 1.0 / (16.0 * SEQ_LEN)
    slow_ceiling = 1.0 / (4.0 * SEQ_LEN)
    fast_floor = 1.0 / 64.0
    fast_ceiling = 0.25
    fractions = jax.random.uniform(key, (D_LRU,), jnp.float32)
    channel_index = jnp.arange(D_LRU)
    parity = (channel_index % 2).astype(jnp.float32)
    plain_floor = minimum_decay_bound + parity * (fast_floor - minimum_decay_bound)
    plain_ceiling = slow_ceiling + parity * (fast_ceiling - slow_ceiling)
    floor_log = jnp.log(plain_floor)
    ceiling_log = jnp.log(plain_ceiling)
    values = jnp.exp(floor_log + fractions * (ceiling_log - floor_log))
    values = jnp.clip(values, plain_floor, plain_ceiling)
    return values.astype(jnp.float32)


def levels(key, shape, split, low, largest):
    def one(position, shards_of):
        steps = jax.random.uniform(jax.random.fold_in(jax.random.fold_in(key, 6), position), (shards_of,), jnp.float32, low / len(split), largest / len(split))
        return jnp.repeat(jnp.exp(steps), shape[position] // shards_of).reshape((-1,) + (1,) * (len(shape) - position - 1))

    level = one(*split[0])
    for cut in split[1:]:
        level = level * one(*cut)
    return level


def centred(key, shape, width, reach, cuts=(), held_as=jnp.bfloat16):
    level = levels(key, shape, cuts, -0.22, 0.18) if cuts else 1.0
    drawn = jax.random.normal(key, shape, jnp.float32) * width * level
    return jnp.minimum(jnp.maximum(drawn, -reach), reach).astype(held_as)


def setup_inputs(seed: int = 0) -> dict:
    streams_of = jax.random.split(jax.random.key(seed), 13)
    tokens = centred(streams_of[0], (SEQS, SEQ_LEN, D), 1.0, 6.0, ((1, 32),))
    norm_gain = jnp.clip(1.0 + 0.1 * jax.random.normal(streams_of[1], (D,), jnp.float32), 0.5, 1.5)
    entry_projection = centred(streams_of[2], (D, D_LRU), D ** -0.5, 0.125, ((1, 8),))
    valve_projection = centred(streams_of[3], (D, D_LRU), D ** -0.5, 0.125, ((1, 8),))
    filter_taps = centred(streams_of[4], (CONV_W, D_LRU), 0.5, 3.0, ((1, 8),), jnp.float32)
    conv_bias = centred(streams_of[5], (D_LRU,), 0.1, 0.6, ((0, 8),), jnp.float32)
    recur_weight = centred(streams_of[6], (BLOCKS, WIDTH_BLOCK, WIDTH_BLOCK), WIDTH_BLOCK ** -0.5, 0.5, ((0, 8),))
    recur_bias = centred(streams_of[7], (D_LRU,), 0.5, 3.0, ((0, 8),), jnp.float32)
    entry_weight = centred(streams_of[8], (BLOCKS, WIDTH_BLOCK, WIDTH_BLOCK), WIDTH_BLOCK ** -0.5, 0.5, ((0, 8),))
    entry_bias = centred(streams_of[9], (D_LRU,), 0.1, 0.6, ((0, 8),), jnp.float32)
    forget_rate = draw_forget_rate(jax.random.fold_in(streams_of[12], 71), 0)
    output_weight = centred(streams_of[11], (D_LRU, D), (D_LRU // 16) ** -0.5, 0.5, ((0, 8),))
    return dict(tokens=tokens, norm_gain=norm_gain, entry_projection=entry_projection, valve_projection=valve_projection, filter_taps=filter_taps, conv_bias=conv_bias, recur_weight=recur_weight, recur_bias=recur_bias, entry_weight=entry_weight, entry_bias=entry_bias, forget_rate=forget_rate, output_weight=output_weight)


epsilon = 1e-06
gate_power = 8.0

def combine_pair(earlier, latter):
    return (earlier[0] * latter[0], latter[0] * earlier[1] + latter[1])

def block_product(convolved, weight):
    grouped = convolved.astype(jnp.float32).reshape(SEQ_LEN, BLOCKS, WIDTH_BLOCK)
    product = jnp.einsum('lhi,hij->lhj', grouped, weight.astype(jnp.float32), precision=lax.Precision.HIGHEST)
    return product.reshape(SEQ_LEN, D_LRU)

def reference(tokens, norm_gain, entry_projection, valve_projection, filter_taps, conv_bias, recur_weight, recur_bias, entry_weight, entry_bias, forget_rate, output_weight):

    def per_sequence(sequence):
        widened = sequence.astype(jnp.float32)
        scaled = widened * lax.rsqrt(lax.optimization_barrier(jnp.mean(widened * widened, axis=-1, keepdims=True)) + epsilon)
        rescaled_values = (scaled * norm_gain).astype(jnp.bfloat16)
        conv_input = jnp.dot(rescaled_values, entry_projection, preferred_element_type=jnp.float32).astype(jnp.bfloat16)
        gate_logits = jnp.dot(rescaled_values, valve_projection, preferred_element_type=jnp.float32).astype(jnp.bfloat16)
        padded = jnp.pad(conv_input, ((CONV_W - 1, 0), (0, 0))).astype(jnp.float32)
        summed = conv_bias + padded[0:SEQ_LEN] * filter_taps[0]
        for offset in range(1, CONV_W):
            summed = summed + padded[offset:offset + SEQ_LEN] * filter_taps[offset]
        convolved = summed.astype(jnp.bfloat16)
        recur_gate = jax.nn.sigmoid(block_product(convolved, recur_weight) + recur_bias)
        entry_gate = jax.nn.sigmoid(block_product(convolved, entry_weight) + entry_bias)
        log_decay = -gate_power * recur_gate * forget_rate
        decay = jnp.exp(log_decay)
        pushed = jnp.sqrt(-jnp.expm1(2.0 * log_decay)) * (entry_gate * convolved.astype(jnp.float32))
        hidden_state = lax.associative_scan(combine_pair, (decay, pushed), axis=0)[1]
        valved_lines = (hidden_state * jax.nn.silu(gate_logits.astype(jnp.float32))).astype(jnp.bfloat16)
        return jnp.dot(valved_lines, output_weight, preferred_element_type=jnp.float32).astype(jnp.bfloat16)
    return lax.map(per_sequence, tokens)
```

```python
import functools

import jax
import jax.numpy as jnp
from jax import lax
from jax.experimental import pallas as pl
from jax.experimental.pallas import tpu as pltpu
from jax.sharding import PartitionSpec as P

epsilon = 1e-06
gate_power = 8.0
MESH = pl.DeviceIdType.MESH
CORES = 2


def kernel(
    SP, TP, Y,
    tok_ref, gain_ref, ew_hbm, vw_hbm, taps_ref, cb_ref, rw_ref, rb_ref, iw_ref, ib_ref, fr_ref, ow_hbm,
    out_ref,
    xg, wf, ew, vw, cbuf, logits, hbuf, dbuf, gbuf, ga, halo, carry,
    tok_send, tok_recv, w_send, wx_send, wc_send, w_recv, a_send, a_recv, c_send, c_recv,
    h_send, h_recv, local,
):
    Z, X = TP // Y, SP // CORES
    sp, tp = lax.axis_index("sp"), lax.axis_index("tp")
    z, y = tp // Y, tp % Y
    x, c = sp // CORES, sp % CORES
    S, T, D = tok_ref.shape
    R = S * T
    C = ew.shape[1]
    B = rw_ref.shape[1]
    K = taps_ref.shape[0]
    H = S * (K - 1)
    HP = halo.shape[0]
    PIECE = wf.shape[2]
    pending = []

    def go(pred, make):
        @pl.when(pred)
        def _():
            make().start()

        pending.append((pred, make))

    loads = [
        pltpu.make_async_copy(ew_hbm, ew, local.at[0]),
        pltpu.make_async_copy(vw_hbm, vw, local.at[1]),
    ]
    for q in range(SP):
        loads.append(
            pltpu.make_async_copy(ow_hbm.at[pl.ds(q * PIECE, PIECE)], wf.at[tp, q], local.at[2 + q])
        )
    for load in loads:
        load.start()

    barrier = pltpu.get_barrier_semaphore()
    for k in range(1, TP):
        pl.semaphore_signal(barrier, inc=1, device_id={"tp": (tp + k) % TP}, device_id_type=MESH)
    for k in range(1, SP):
        pl.semaphore_signal(barrier, inc=1, device_id={"sp": (sp + k) % SP}, device_id_type=MESH)

    r_i = lax.broadcasted_iota(jnp.int32, (R, R), 0)
    c_i = lax.broadcasted_iota(jnp.int32, (R, R), 1)
    to_time = jnp.where(c_i == (r_i % S) * T + r_i // S, 1.0, 0.0).astype(jnp.bfloat16)
    to_seq = jnp.where(r_i == (c_i % S) * T + c_i // S, 1.0, 0.0).astype(jnp.bfloat16)

    wide = tok_ref[...].reshape(R, D).astype(jnp.float32)
    scaled = wide * lax.rsqrt(jnp.mean(wide * wide, axis=-1, keepdims=True) + epsilon)
    normed = (scaled * gain_ref[...]).astype(jnp.bfloat16)
    xg[tp] = jnp.dot(to_time, normed, preferred_element_type=jnp.float32).astype(jnp.bfloat16)

    pl.semaphore_wait(barrier, TP - 1 + SP - 1)

    def tok_copy(slot, target, way):
        return pltpu.make_async_remote_copy(
            xg.at[slot], xg.at[slot], tok_send.at[slot, way], tok_recv.at[slot],
            device_id={"tp": target}, device_id_type=MESH)

    def w_copy(slot, target, way):
        return pltpu.make_async_remote_copy(
            wf.at[slot, sp], wf.at[slot, sp], w_send.at[slot, way], w_recv.at[slot, sp],
            device_id={"tp": target}, device_id_type=MESH)

    def x_copy(slot, xx, step, way):
        q = xx * CORES + c
        return pltpu.make_async_remote_copy(
            wf.at[slot, q], wf.at[slot, q], wx_send.at[slot, xx, way], w_recv.at[slot, q],
            device_id={"sp": sp + step * CORES}, device_id_type=MESH)

    def core_copy(slot, xx):
        q = xx * CORES + c
        return pltpu.make_async_remote_copy(
            wf.at[slot, q], wf.at[slot, q], wc_send.at[slot, xx], w_recv.at[slot, q],
            device_id={"sp": x * CORES + 1 - c}, device_id_type=MESH)

    def project(slot):
        a = xg[slot]
        base = pl.multiple_of(slot * R + HP, 16)
        cin = jnp.dot(a, ew[...], preferred_element_type=jnp.float32)
        cbuf[pl.ds(base, R), :] = cin.astype(jnp.bfloat16).astype(jnp.float32)
        lg = jnp.dot(a, vw[...], preferred_element_type=jnp.float32)
        logits[slot] = lg.astype(jnp.bfloat16)

    def inside(v, n):
        return (v >= 0) & (v < n)

    def spread(copy, slot, valid, zz_step, both):
        for way, step in ((0, 1), (1, -1)):
            if both or step == zz_step:
                go(valid & inside(z + step, Z), functools.partial(copy, slot, tp + step * Y, way))
        for way, step in ((2, 1), (3, -1)):
            go(valid & inside(y + step, Y), functools.partial(copy, slot, tp + step, way))

    def received(buf_at, sem):
        pltpu.make_async_copy(buf_at, buf_at, sem).wait()

    spread(tok_copy, tp, z >= 0, 0, True)
    loads[0].wait()
    loads[1].wait()
    for q in range(SP):
        loads[2 + q].wait()

    def x_spread(slot, valid):
        for way, step in ((0, 1), (1, -1)):
            go(valid & inside(x + step, X), functools.partial(x_copy, slot, x, step, way))
        go(valid, functools.partial(core_copy, slot, x))

    project(tp)

    def along_z(d, copy, arrived, after):
        for step in (1, -1):
            zz = z - step * d
            valid = inside(zz, Z)
            slot = zz * Y + y

            @pl.when(valid)
            def _(slot=slot):
                arrived(slot)

            spread(copy, slot, valid, step, False)
            after(slot, valid)

    def along_y(copy, arrived, after):
        for e in range(1, Y):
            for d in range(Z):
                for zs in (1, -1) if d else (1,):
                    for step in (1, -1):
                        zz, yy = z - zs * d, y - step * e
                        valid = inside(zz, Z) & inside(yy, Y)
                        slot = zz * Y + yy

                        @pl.when(valid)
                        def _(slot=slot):
                            arrived(slot)

                        go(
                            valid & inside(y + step, Y),
                            functools.partial(copy, slot, tp + step, 2 if step == 1 else 3),
                        )
                        after(slot, valid)

    def tok_arrived(slot):
        received(xg.at[slot], tok_recv.at[slot])

    def tok_after(slot, valid):
        @pl.when(valid)
        def _():
            project(slot)

    def w_arrived(slot):
        received(wf.at[slot, sp], w_recv.at[slot, sp])

    for d in range(1, Z):
        along_z(d, tok_copy, tok_arrived, tok_after)
    spread(w_copy, tp, z >= 0, 0, True)
    for d in range(1, Z - 1):
        along_z(d, w_copy, w_arrived, x_spread)
    along_y(tok_copy, tok_arrived, tok_after)

    def halo_copy():
        return pltpu.make_async_remote_copy(
            cbuf.at[pl.ds(TP * R, HP)], halo, h_send, h_recv,
            device_id={"sp": sp + 1}, device_id_type=MESH)

    go(sp + 1 < SP, halo_copy)

    @pl.when(sp == 0)
    def _():
        cbuf[pl.ds(0, HP), :] = jnp.zeros((HP, C), jnp.float32)

    @pl.when(sp > 0)
    def _():
        received(halo, h_recv)
        cbuf[pl.ds(0, HP), :] = halo[...]

    def spreadrows(v):
        return jnp.broadcast_to(
            jnp.concatenate([v] * (8 // S), axis=0)[None], (R // 8, 8, B)
        ).reshape(R, B)

    for b in range(C // B):
        cols = slice(b * B, (b + 1) * B)

        def chunk(j, state, b=b, cols=cols):
            dc, hc = state
            blk = cbuf[pl.ds(pl.multiple_of(j * R, 16), R + HP), cols]
            conv = cb_ref[:, cols]
            for k in range(K):
                o = HP - H + S * k
                conv = conv + blk[o : o + R] * taps_ref[k : k + 1, cols]
            cv = conv.astype(jnp.bfloat16)
            rg = jax.nn.sigmoid(
                jnp.dot(cv, rw_ref[b], preferred_element_type=jnp.float32) + rb_ref[:, cols])
            ig = jax.nn.sigmoid(
                jnp.dot(cv, iw_ref[b], preferred_element_type=jnp.float32) + ib_ref[:, cols])
            ld = -gate_power * rg * fr_ref[:, cols]
            a = jnp.exp(ld)
            v = jnp.sqrt(-jnp.tanh(ld) * (a * a + 1.0)) * (ig * cv.astype(jnp.float32))
            d = S
            while d < R:
                a_s = jnp.concatenate([jnp.ones((d, B), jnp.float32), a[: R - d]], axis=0)
                v_s = jnp.concatenate([jnp.zeros((d, B), jnp.float32), v[: R - d]], axis=0)
                v = a * v_s + v
                a = a * a_s
                d *= 2
            v = v + a * spreadrows(hc)
            a = a * spreadrows(dc)
            hbuf[j, :, cols] = v
            dbuf[j, :, cols] = a
            return a[R - S :], v[R - S :]

        dc, hc = lax.fori_loop(
            0, TP, chunk, (jnp.ones((S, B), jnp.float32), jnp.zeros((S, B), jnp.float32)))
        carry[sp, 0, :, cols] = dc
        carry[sp, 1, :, cols] = hc

    def carry_copy(k):
        return pltpu.make_async_remote_copy(
            carry.at[sp], carry.at[sp], c_send.at[k], c_recv.at[sp],
            device_id={"sp": (sp + k) % SP}, device_id_type=MESH)

    for k in range(1, SP):
        go(sp >= 0, functools.partial(carry_copy, k))
    if Z > 1:
        along_z(Z - 1, w_copy, w_arrived, x_spread)
    for k in range(1, SP):
        other = (sp + k) % SP
        received(carry.at[other], c_recv.at[other])
    entering = jnp.zeros((S, C), jnp.float32)
    for k in range(SP - 1):
        entering = jnp.where(k < sp, carry[k, 0] * entering + carry[k, 1], entering)

    rows = jnp.broadcast_to(
        jnp.concatenate([entering] * (8 // S), axis=0)[None], (R // 8, 8, C)
    ).reshape(R, C)

    def gate(j):
        h = hbuf[j] + dbuf[j] * rows
        g = logits[j].astype(jnp.float32)
        gated = (h * (g / (1.0 + jnp.exp(-g)))).astype(jnp.bfloat16)
        return jnp.dot(to_seq, gated, preferred_element_type=jnp.float32).astype(jnp.bfloat16)

    def a_copy(k):
        target = (tp + k) % TP
        return pltpu.make_async_remote_copy(
            gbuf.at[target], ga.at[tp], a_send.at[k], a_recv.at[tp],
            device_id={"tp": target}, device_id_type=MESH)

    for k in range(1, TP):
        j = (tp + k) % TP
        gbuf[j] = gate(j)
        go(tp >= 0, functools.partial(a_copy, k))
    ga[tp] = gate(tp)

    along_y(w_copy, w_arrived, x_spread)

    for k in range(1, TP):
        i = (tp + k) % TP
        for d in range(1, X):
            for step in (1, -1):
                xx = x - step * d
                valid = inside(xx, X)
                q = xx * CORES + c

                @pl.when(valid)
                def _(i=i, q=q):
                    received(wf.at[i, q], w_recv.at[i, q])

                go(
                    valid & inside(x + step, X),
                    functools.partial(x_copy, i, xx, step, 0 if step == 1 else 1),
                )
                go(valid, functools.partial(core_copy, i, xx))
    for k in range(1, TP):
        i = (tp + k) % TP
        for xx in range(X):
            q = xx * CORES + 1 - c
            received(wf.at[i, q], w_recv.at[i, q])

    for k in range(1, TP):
        other = (tp + k) % TP
        received(ga.at[other], a_recv.at[other])

    tile = 512 if D % 512 == 0 else D
    for n in range(D // tile):
        at = slice(n * tile, (n + 1) * tile)
        acc = jnp.zeros((R, tile), jnp.float32)
        for i in range(TP):
            acc = acc + jnp.dot(
                ga[i], wf[i, :, :, at].reshape(C, tile), preferred_element_type=jnp.float32)
        out_ref[:, :, at] = acc.astype(jnp.bfloat16).reshape(S, T, tile)

    for pred, make in pending:

        @pl.when(pred)
        def _(make=make):
            make().wait_send()


def per_device(
    SP, TP, Y,
    tokens, norm_gain, entry_projection, valve_projection, filter_taps, conv_bias,
    recur_weight, recur_bias, entry_weight, entry_bias, forget_rate, output_weight,
):
    S, T, D = tokens.shape
    R = S * T
    C = entry_projection.shape[1]
    HP = 16
    vmem = pl.BlockSpec(memory_space=pltpu.VMEM)
    hbm = pl.BlockSpec(memory_space=pl.ANY)
    f32, bf16 = jnp.float32, jnp.bfloat16
    dma = pltpu.SemaphoreType.DMA
    X = SP // CORES
    return pl.pallas_call(
        functools.partial(kernel, SP, TP, Y),
        out_shape=jax.ShapeDtypeStruct(tokens.shape, bf16),
        in_specs=[vmem, vmem, hbm, hbm] + [vmem] * 7 + [hbm],
        out_specs=vmem,
        scratch_shapes=[
            pltpu.VMEM((TP, R, D), bf16),
            pltpu.VMEM((TP, SP, C // SP, D), bf16),
            pltpu.VMEM((D, C), bf16),
            pltpu.VMEM((D, C), bf16),
            pltpu.VMEM((TP * R + HP, C), f32),
            pltpu.VMEM((TP, R, C), bf16),
            pltpu.VMEM((TP, R, C), f32),
            pltpu.VMEM((TP, R, C), f32),
            pltpu.VMEM((TP, R, C), bf16),
            pltpu.VMEM((TP, R, C), bf16),
            pltpu.VMEM((HP, C), f32),
            pltpu.VMEM((SP, 2, S, C), f32),
            dma((TP, 4)), dma((TP,)),
            dma((TP, 4)), dma((TP, X, 2)), dma((TP, X)), dma((TP, SP)),
            dma((TP,)), dma((TP,)), dma((SP,)), dma((SP,)),
            dma, dma, dma((2 + SP,)),
        ],
        compiler_params=pltpu.CompilerParams(
            collective_id=0, has_side_effects=True, vmem_limit_bytes=60 * 1024 * 1024
        ),
    )(
        tokens, norm_gain[None], entry_projection, valve_projection, filter_taps, conv_bias[None],
        recur_weight, recur_bias[None], entry_weight, entry_bias[None], forget_rate[None],
        output_weight,
    )


def solution(mesh):
    SP, TP = mesh.shape["sp"], mesh.shape["tp"]
    try:
        Y = len({tuple(d.coords)[1] for d in mesh.devices.flat})
    except AttributeError:
        Y = 1
    return jax.shard_map(
        functools.partial(per_device, SP, TP, Y),
        mesh=mesh,
        in_specs=(
            P(None, ("sp", "tp"), None),
            P(),
            P(None, "tp"),
            P(None, "tp"),
            P(None, "tp"),
            P("tp"),
            P("tp", None, None),
            P("tp"),
            P("tp", None, None),
            P("tp"),
            P("tp"),
            P("tp", None),
        ),
        out_specs=P(None, ("sp", "tp"), None),
        check_vma=False,
    )
```

```python
import functools

import jax
import jax.numpy as jnp
from jax import lax
from jax.experimental import pallas as pl
from jax.experimental.pallas import tpu as pltpu
from jax.sharding import PartitionSpec as P

epsilon = 1e-06
gate_power = 8.0
MESH = pl.DeviceIdType.MESH
CORES = 2


def kernel(
    SP, TP, Y,
    tok_ref, gain_ref, ew_hbm, vw_hbm, taps_ref, cb_ref, rw_ref, rb_ref, iw_ref, ib_ref, fr_ref, ow_hbm,
    out_ref,
    xg, wf, ew, vw, cbuf, logits, hbuf, dbuf, gbuf, ga, halo, carry,
    tok_send, tok_recv, w_send, wx_send, wc_send, w_recv, a_send, a_recv, c_send, c_recv,
    h_send, h_recv, p_send, p_recv, local, pbuf, rbuf,
):
    Z, X = TP // Y, SP // CORES
    sp, tp = lax.axis_index("sp"), lax.axis_index("tp")
    z, y = tp // Y, tp % Y
    x, c = sp // CORES, sp % CORES
    S, T, D = tok_ref.shape
    R = S * T
    C = ew.shape[1]
    B = rw_ref.shape[1]
    K = taps_ref.shape[0]
    H = S * (K - 1)
    HP = halo.shape[0]
    PIECE = wf.shape[2]
    pending = []

    def go(pred, make):
        @pl.when(pred)
        def _():
            make().start()

        pending.append((pred, make))

    loads = [
        pltpu.make_async_copy(ew_hbm, ew, local.at[0]),
        pltpu.make_async_copy(vw_hbm, vw, local.at[1]),
    ]
    for q in range(SP):
        loads.append(
            pltpu.make_async_copy(ow_hbm.at[pl.ds(q * PIECE, PIECE)], wf.at[z, q], local.at[2 + q])
        )
    for load in loads:
        load.start()

    barrier = pltpu.get_barrier_semaphore()
    for k in range(1, TP):
        pl.semaphore_signal(barrier, inc=1, device_id={"tp": (tp + k) % TP}, device_id_type=MESH)
    for k in range(1, SP):
        pl.semaphore_signal(barrier, inc=1, device_id={"sp": (sp + k) % SP}, device_id_type=MESH)

    r_i = lax.broadcasted_iota(jnp.int32, (R, R), 0)
    c_i = lax.broadcasted_iota(jnp.int32, (R, R), 1)
    to_time = jnp.where(c_i == (r_i % S) * T + r_i // S, 1.0, 0.0).astype(jnp.bfloat16)
    to_seq = jnp.where(r_i == (c_i % S) * T + c_i // S, 1.0, 0.0).astype(jnp.bfloat16)

    wide = tok_ref[...].reshape(R, D).astype(jnp.float32)
    scaled = wide * lax.rsqrt(jnp.mean(wide * wide, axis=-1, keepdims=True) + epsilon)
    normed = (scaled * gain_ref[...]).astype(jnp.bfloat16)
    xg[tp] = jnp.dot(to_time, normed, preferred_element_type=jnp.float32).astype(jnp.bfloat16)

    pl.semaphore_wait(barrier, TP - 1 + SP - 1)

    def tok_copy(slot, target, way):
        return pltpu.make_async_remote_copy(
            xg.at[slot], xg.at[slot], tok_send.at[slot, way], tok_recv.at[slot],
            device_id={"tp": target}, device_id_type=MESH)

    def w_copy(slot, target, way):
        return pltpu.make_async_remote_copy(
            wf.at[slot, sp], wf.at[slot, sp], w_send.at[slot, way], w_recv.at[slot, sp],
            device_id={"tp": target}, device_id_type=MESH)

    def x_copy(slot, xx, step, way):
        q = xx * CORES + c
        return pltpu.make_async_remote_copy(
            wf.at[slot, q], wf.at[slot, q], wx_send.at[slot, xx, way], w_recv.at[slot, q],
            device_id={"sp": sp + step * CORES}, device_id_type=MESH)

    def core_copy(slot, xx):
        q = xx * CORES + c
        return pltpu.make_async_remote_copy(
            wf.at[slot, q], wf.at[slot, q], wc_send.at[slot, xx], w_recv.at[slot, q],
            device_id={"sp": x * CORES + 1 - c}, device_id_type=MESH)

    def project(slot):
        a = xg[slot]
        base = pl.multiple_of(slot * R + HP, 16)
        cin = jnp.dot(a, ew[...], preferred_element_type=jnp.float32)
        cbuf[pl.ds(base, R), :] = cin.astype(jnp.bfloat16).astype(jnp.float32)
        lg = jnp.dot(a, vw[...], preferred_element_type=jnp.float32)
        logits[slot] = lg.astype(jnp.bfloat16)

    def inside(v, n):
        return (v >= 0) & (v < n)

    def pass_z(copy, slot, valid, step):
        way = 0 if step == 1 else 1
        go(valid & inside(z + step, Z), functools.partial(copy, slot, tp + step * Y, way))

    def pass_y(slot, valid):
        for way, step in ((2, 1), (3, -1)):
            go(valid & inside(y + step, Y), functools.partial(tok_copy, slot, tp + step, way))

    def received(buf_at, sem):
        pltpu.make_async_copy(buf_at, buf_at, sem).wait()

    for step in (1, -1):
        pass_z(tok_copy, tp, z >= 0, step)
    pass_y(tp, z >= 0)
    for load in loads:
        load.wait()
    project(tp)

    def own_piece(d):
        pass_z(w_copy, z, z == d, 1)
        pass_z(w_copy, z, Z - 1 - z == d, -1)

    own_piece(0)

    def x_spread(slot, valid):
        for way, step in ((0, 1), (1, -1)):
            go(valid & inside(x + step, X), functools.partial(x_copy, slot, x, step, way))
        go(valid, functools.partial(core_copy, slot, x))

    def along_z(d, copy, slot_of, arrived, after):
        for step in (1, -1):
            zz = z - step * d
            valid = inside(zz, Z)
            slot = slot_of(zz)

            @pl.when(valid)
            def _(slot=slot):
                arrived(slot)

            pass_z(copy, slot, valid, step)
            after(slot, valid)

    def tok_arrived(slot):
        received(xg.at[slot], tok_recv.at[slot])

    def tok_project(slot, valid):
        @pl.when(valid)
        def _():
            project(slot)

    def tok_after(slot, valid):
        pass_y(slot, valid)
        tok_project(slot, valid)

    def w_arrived(slot):
        received(wf.at[slot, sp], w_recv.at[slot, sp])

    for d in range(1, Z):
        along_z(d, tok_copy, lambda zz: zz * Y + y, tok_arrived, tok_after)
        own_piece(d)
    for d in range(1, Z - 1):
        along_z(d, w_copy, lambda zz: zz, w_arrived, x_spread)
    for e in range(1, Y):
        for d in range(Z):
            for zs in (1, -1) if d else (1,):
                for step in (1, -1):
                    zz, yy = z - zs * d, y - step * e
                    valid = inside(zz, Z) & inside(yy, Y)
                    slot = zz * Y + yy

                    @pl.when(valid)
                    def _(slot=slot):
                        tok_arrived(slot)

                    go(
                        valid & inside(y + step, Y),
                        functools.partial(tok_copy, slot, tp + step, 2 if step == 1 else 3),
                    )
                    tok_project(slot, valid)

    def halo_copy():
        return pltpu.make_async_remote_copy(
            cbuf.at[pl.ds(TP * R, HP)], halo, h_send, h_recv,
            device_id={"sp": sp + 1}, device_id_type=MESH)

    go(sp + 1 < SP, halo_copy)

    @pl.when(sp == 0)
    def _():
        cbuf[pl.ds(0, HP), :] = jnp.zeros((HP, C), jnp.float32)

    @pl.when(sp > 0)
    def _():
        received(halo, h_recv)
        cbuf[pl.ds(0, HP), :] = halo[...]

    def spreadrows(v):
        return jnp.broadcast_to(
            jnp.concatenate([v] * (8 // S), axis=0)[None], (R // 8, 8, B)
        ).reshape(R, B)

    for b in range(C // B):
        cols = slice(b * B, (b + 1) * B)

        def chunk(j, state, b=b, cols=cols):
            dc, hc = state
            blk = cbuf[pl.ds(pl.multiple_of(j * R, 16), R + HP), cols]
            conv = cb_ref[:, cols]
            for k in range(K):
                o = HP - H + S * k
                conv = conv + blk[o : o + R] * taps_ref[k : k + 1, cols]
            cv = conv.astype(jnp.bfloat16)
            rg = jax.nn.sigmoid(
                jnp.dot(cv, rw_ref[b], preferred_element_type=jnp.float32) + rb_ref[:, cols])
            ig = jax.nn.sigmoid(
                jnp.dot(cv, iw_ref[b], preferred_element_type=jnp.float32) + ib_ref[:, cols])
            ld = -gate_power * rg * fr_ref[:, cols]
            a = jnp.exp(ld)
            v = jnp.sqrt(-jnp.tanh(ld) * (a * a + 1.0)) * (ig * cv.astype(jnp.float32))
            d = S
            while d < R:
                a_s = jnp.concatenate([jnp.ones((d, B), jnp.float32), a[: R - d]], axis=0)
                v_s = jnp.concatenate([jnp.zeros((d, B), jnp.float32), v[: R - d]], axis=0)
                v = a * v_s + v
                a = a * a_s
                d *= 2
            v = v + a * spreadrows(hc)
            a = a * spreadrows(dc)
            hbuf[j, :, cols] = v
            dbuf[j, :, cols] = a
            return a[R - S :], v[R - S :]

        dc, hc = lax.fori_loop(
            0, TP, chunk, (jnp.ones((S, B), jnp.float32), jnp.zeros((S, B), jnp.float32)))
        carry[sp, 0, :, cols] = dc
        carry[sp, 1, :, cols] = hc

    def carry_copy(k):
        return pltpu.make_async_remote_copy(
            carry.at[sp], carry.at[sp], c_send.at[k], c_recv.at[sp],
            device_id={"sp": (sp + k) % SP}, device_id_type=MESH)

    for k in range(1, SP):
        go(sp >= 0, functools.partial(carry_copy, k))
    if Z > 1:
        along_z(Z - 1, w_copy, lambda zz: zz, w_arrived, x_spread)
    for k in range(1, SP):
        other = (sp + k) % SP
        received(carry.at[other], c_recv.at[other])
    entering = jnp.zeros((S, C), jnp.float32)
    for k in range(SP - 1):
        entering = jnp.where(k < sp, carry[k, 0] * entering + carry[k, 1], entering)

    rows = jnp.broadcast_to(
        jnp.concatenate([entering] * (8 // S), axis=0)[None], (R // 8, 8, C)
    ).reshape(R, C)

    def gate(j):
        h = hbuf[j] + dbuf[j] * rows
        g = logits[j].astype(jnp.float32)
        gated = (h * (g / (1.0 + jnp.exp(-g)))).astype(jnp.bfloat16)
        return jnp.dot(to_seq, gated, preferred_element_type=jnp.float32).astype(jnp.bfloat16)

    def a_copy(k):
        target = (z + k) % Z
        return pltpu.make_async_remote_copy(
            gbuf.at[pl.ds(target * Y, Y)], ga.at[z], a_send.at[k], a_recv.at[z],
            device_id={"tp": target * Y + y}, device_id_type=MESH)

    for k in range(1, Z):
        for yy in range(Y):
            j = (z + k) % Z * Y + yy
            gbuf[j] = gate(j)
        go(z >= 0, functools.partial(a_copy, k))
    for yy in range(Y):
        ga[z, yy] = gate(z * Y + yy)

    for k in range(1, Z):
        i = (z + k) % Z
        for d in range(1, X):
            for step in (1, -1):
                xx = x - step * d
                valid = inside(xx, X)
                q = xx * CORES + c

                @pl.when(valid)
                def _(i=i, q=q):
                    received(wf.at[i, q], w_recv.at[i, q])

                go(
                    valid & inside(x + step, X),
                    functools.partial(x_copy, i, xx, step, 0 if step == 1 else 1),
                )
                go(valid, functools.partial(core_copy, i, xx))
    for k in range(1, Z):
        i = (z + k) % Z
        for xx in range(X):
            q = xx * CORES + 1 - c
            received(wf.at[i, q], w_recv.at[i, q])

    for k in range(1, Z):
        other = (z + k) % Z
        received(ga.at[other], a_recv.at[other])

    tile = pbuf.shape[3]
    tiles = D // tile

    def line_sum(yy, n):
        at = slice(n * tile, (n + 1) * tile)
        acc = jnp.zeros((R, tile), jnp.float32)
        for i in range(Z):
            acc = acc + jnp.dot(
                ga[i, yy], wf[i, :, :, at].reshape(C, tile), preferred_element_type=jnp.float32)
        return acc

    def p_copy(k, n):
        return pltpu.make_async_remote_copy(
            pbuf.at[k, n], rbuf.at[k, n], p_send.at[k, n], p_recv.at[k, n],
            device_id={"tp": z * Y + (y + k) % Y}, device_id_type=MESH)

    for n in range(tiles):
        for k in range(1, Y):
            pbuf[k, n] = line_sum((y + k) % Y, n).astype(jnp.bfloat16)
            go(z >= 0, functools.partial(p_copy, k, n))
    own = [line_sum(y, n) for n in range(tiles)]
    for n in range(tiles):
        total = own[n]
        for k in range(1, Y):
            received(rbuf.at[k, n], p_recv.at[k, n])
            total = total + rbuf[k, n].astype(jnp.float32)
        out_ref[:, :, n * tile : (n + 1) * tile] = total.astype(jnp.bfloat16).reshape(S, T, tile)

    for pred, make in pending:

        @pl.when(pred)
        def _(make=make):
            make().wait_send()


def per_device(
    SP, TP, Y,
    tokens, norm_gain, entry_projection, valve_projection, filter_taps, conv_bias,
    recur_weight, recur_bias, entry_weight, entry_bias, forget_rate, output_weight,
):
    S, T, D = tokens.shape
    R = S * T
    C = entry_projection.shape[1]
    HP = 16
    vmem = pl.BlockSpec(memory_space=pltpu.VMEM)
    hbm = pl.BlockSpec(memory_space=pl.ANY)
    f32, bf16 = jnp.float32, jnp.bfloat16
    dma = pltpu.SemaphoreType.DMA
    X, Z = SP // CORES, TP // Y
    tile = 512 if D % 512 == 0 else D
    return pl.pallas_call(
        functools.partial(kernel, SP, TP, Y),
        out_shape=jax.ShapeDtypeStruct(tokens.shape, bf16),
        in_specs=[vmem, vmem, hbm, hbm] + [vmem] * 7 + [hbm],
        out_specs=vmem,
        scratch_shapes=[
            pltpu.VMEM((TP, R, D), bf16),
            pltpu.VMEM((Z, SP, C // SP, D), bf16),
            pltpu.VMEM((D, C), bf16),
            pltpu.VMEM((D, C), bf16),
            pltpu.VMEM((TP * R + HP, C), f32),
            pltpu.VMEM((TP, R, C), bf16),
            pltpu.VMEM((TP, R, C), f32),
            pltpu.VMEM((TP, R, C), f32),
            pltpu.VMEM((TP, R, C), bf16),
            pltpu.VMEM((Z, Y, R, C), bf16),
            pltpu.VMEM((HP, C), f32),
            pltpu.VMEM((SP, 2, S, C), f32),
            dma((TP, 4)), dma((TP,)),
            dma((Z, 2)), dma((Z, X, 2)), dma((Z, X)), dma((Z, SP)),
            dma((Z,)), dma((Z,)), dma((SP,)), dma((SP,)),
            dma, dma, dma((Y, D // tile)), dma((Y, D // tile)), dma((2 + SP,)),
            pltpu.VMEM((Y, D // tile, R, tile), bf16),
            pltpu.VMEM((Y, D // tile, R, tile), bf16),
        ],
        compiler_params=pltpu.CompilerParams(
            collective_id=0, has_side_effects=True, vmem_limit_bytes=60 * 1024 * 1024
        ),
    )(
        tokens, norm_gain[None], entry_projection, valve_projection, filter_taps, conv_bias[None],
        recur_weight, recur_bias[None], entry_weight, entry_bias[None], forget_rate[None],
        output_weight,
    )


def solution(mesh):
    SP, TP = mesh.shape["sp"], mesh.shape["tp"]
    try:
        Y = len({tuple(d.coords)[1] for d in mesh.devices.flat})
    except AttributeError:
        Y = 1
    return jax.shard_map(
        functools.partial(per_device, SP, TP, Y),
        mesh=mesh,
        in_specs=(
            P(None, ("sp", "tp"), None),
            P(),
            P(None, "tp"),
            P(None, "tp"),
            P(None, "tp"),
            P("tp"),
            P("tp", None, None),
            P("tp"),
            P("tp", None, None),
            P("tp"),
            P("tp"),
            P("tp", None),
        ),
        out_specs=P(None, ("sp", "tp"), None),
        check_vma=False,
    )
```

```python
import functools

import jax
import jax.numpy as jnp
from jax import lax
from jax.experimental import pallas as pl
from jax.experimental.pallas import tpu as pltpu
from jax.sharding import PartitionSpec as P

epsilon = 1e-06
gate_power = 8.0
MESH = pl.DeviceIdType.MESH
CORES = 2


def kernel(
    SP, TP, Y,
    tok_ref, gain_ref, ew_hbm, vw_hbm, taps_ref, cb_ref, rw_ref, rb_ref, iw_ref, ib_ref, fr_ref, ow_hbm,
    out_ref,
    xg, wf, ew, vw, cbuf, logits, hbuf, dbuf, gbuf, ga, halo, carry,
    tok_send, tok_recv, w_send, wx_send, wc_send, w_recv, a_send, a_recv, c_send, c_recv,
    h_send, h_recv, p_send, p_recv, local, pbuf, rbuf,
):
    Z, X = TP // Y, SP // CORES
    sp, tp = lax.axis_index("sp"), lax.axis_index("tp")
    z, y = tp // Y, tp % Y
    x, c = sp // CORES, sp % CORES
    S, T, D = tok_ref.shape
    R = S * T
    C = ew.shape[1]
    B = rw_ref.shape[1]
    K = taps_ref.shape[0]
    H = S * (K - 1)
    HP = halo.shape[0]
    PIECE = wf.shape[2]
    pending = []

    def go(pred, make):
        @pl.when(pred)
        def _():
            make().start()

        pending.append((pred, make))

    loads = [
        pltpu.make_async_copy(ew_hbm, ew, local.at[0]),
        pltpu.make_async_copy(vw_hbm, vw, local.at[1]),
    ]
    for q in range(SP):
        loads.append(
            pltpu.make_async_copy(ow_hbm.at[pl.ds(q * PIECE, PIECE)], wf.at[z, q], local.at[2 + q])
        )
    for load in loads:
        load.start()

    barrier = pltpu.get_barrier_semaphore()
    for k in range(1, TP):
        pl.semaphore_signal(barrier, inc=1, device_id={"tp": (tp + k) % TP}, device_id_type=MESH)
    for k in range(1, SP):
        pl.semaphore_signal(barrier, inc=1, device_id={"sp": (sp + k) % SP}, device_id_type=MESH)

    r_i = lax.broadcasted_iota(jnp.int32, (R, R), 0)
    c_i = lax.broadcasted_iota(jnp.int32, (R, R), 1)
    to_time = jnp.where(c_i == (r_i % S) * T + r_i // S, 1.0, 0.0).astype(jnp.bfloat16)
    to_seq = jnp.where(r_i == (c_i % S) * T + c_i // S, 1.0, 0.0).astype(jnp.bfloat16)

    wide = tok_ref[...].reshape(R, D).astype(jnp.float32)
    scaled = wide * lax.rsqrt(jnp.mean(wide * wide, axis=-1, keepdims=True) + epsilon)
    normed = (scaled * gain_ref[...]).astype(jnp.bfloat16)
    xg[tp] = jnp.dot(to_time, normed, preferred_element_type=jnp.float32).astype(jnp.bfloat16)

    pl.semaphore_wait(barrier, TP - 1 + SP - 1)

    def tok_copy(slot, target, way):
        return pltpu.make_async_remote_copy(
            xg.at[slot], xg.at[slot], tok_send.at[slot, way], tok_recv.at[slot],
            device_id={"tp": target}, device_id_type=MESH)

    def w_copy(slot, target, way):
        return pltpu.make_async_remote_copy(
            wf.at[slot, sp], wf.at[slot, sp], w_send.at[slot, way], w_recv.at[slot, sp],
            device_id={"tp": target}, device_id_type=MESH)

    def x_copy(slot, xx, step, way):
        q = xx * CORES + c
        return pltpu.make_async_remote_copy(
            wf.at[slot, q], wf.at[slot, q], wx_send.at[slot, xx, way], w_recv.at[slot, q],
            device_id={"sp": sp + step * CORES}, device_id_type=MESH)

    def core_copy(slot, xx):
        q = xx * CORES + c
        return pltpu.make_async_remote_copy(
            wf.at[slot, q], wf.at[slot, q], wc_send.at[slot, xx], w_recv.at[slot, q],
            device_id={"sp": x * CORES + 1 - c}, device_id_type=MESH)

    def project(slot):
        a = xg[slot]
        base = pl.multiple_of(slot * R + HP, 16)
        cin = jnp.dot(a, ew[...], preferred_element_type=jnp.float32)
        cbuf[pl.ds(base, R), :] = cin.astype(jnp.bfloat16).astype(jnp.float32)
        lg = jnp.dot(a, vw[...], preferred_element_type=jnp.float32)
        logits[slot] = lg.astype(jnp.bfloat16)

    def inside(v, n):
        return (v >= 0) & (v < n)

    def pass_z(copy, slot, valid, step):
        way = 0 if step == 1 else 1
        go(valid & inside(z + step, Z), functools.partial(copy, slot, tp + step * Y, way))

    def pass_y(slot, valid):
        for way, step in ((2, 1), (3, -1)):
            go(valid & inside(y + step, Y), functools.partial(tok_copy, slot, tp + step, way))

    def received(buf_at, sem):
        pltpu.make_async_copy(buf_at, buf_at, sem).wait()

    for step in (1, -1):
        pass_z(tok_copy, tp, z >= 0, step)
    pass_y(tp, z >= 0)
    for load in loads:
        load.wait()
    project(tp)

    def own_piece(d):
        pass_z(w_copy, z, z == d, 1)
        pass_z(w_copy, z, Z - 1 - z == d, -1)

    own_piece(0)

    def x_spread(slot, valid):
        for way, step in ((0, 1), (1, -1)):
            go(valid & inside(x + step, X), functools.partial(x_copy, slot, x, step, way))
        go(valid, functools.partial(core_copy, slot, x))

    def along_z(d, copy, slot_of, arrived, after):
        for step in (1, -1):
            zz = z - step * d
            valid = inside(zz, Z)
            slot = slot_of(zz)

            @pl.when(valid)
            def _(slot=slot):
                arrived(slot)

            pass_z(copy, slot, valid, step)
            after(slot, valid)

    def tok_arrived(slot):
        received(xg.at[slot], tok_recv.at[slot])

    def tok_project(slot, valid):
        @pl.when(valid)
        def _():
            project(slot)

    def tok_after(slot, valid):
        pass_y(slot, valid)
        tok_project(slot, valid)

    def w_arrived(slot):
        received(wf.at[slot, sp], w_recv.at[slot, sp])

    for d in range(1, Z):
        along_z(d, tok_copy, lambda zz: zz * Y + y, tok_arrived, tok_after)
        own_piece(d)
    for d in range(1, Z - 1):
        along_z(d, w_copy, lambda zz: zz, w_arrived, x_spread)
    for e in range(1, Y):
        for d in range(Z):
            for zs in (1, -1) if d else (1,):
                for step in (1, -1):
                    zz, yy = z - zs * d, y - step * e
                    valid = inside(zz, Z) & inside(yy, Y)
                    slot = zz * Y + yy

                    @pl.when(valid)
                    def _(slot=slot):
                        tok_arrived(slot)

                    go(
                        valid & inside(y + step, Y),
                        functools.partial(tok_copy, slot, tp + step, 2 if step == 1 else 3),
                    )
                    tok_project(slot, valid)

    def halo_copy():
        return pltpu.make_async_remote_copy(
            cbuf.at[pl.ds(TP * R, HP)], halo, h_send, h_recv,
            device_id={"sp": sp + 1}, device_id_type=MESH)

    go(sp + 1 < SP, halo_copy)

    @pl.when(sp == 0)
    def _():
        cbuf[pl.ds(0, HP), :] = jnp.zeros((HP, C), jnp.float32)

    @pl.when(sp > 0)
    def _():
        received(halo, h_recv)
        cbuf[pl.ds(0, HP), :] = halo[...]

    def spreadrows(v):
        return jnp.broadcast_to(
            jnp.concatenate([v] * (8 // S), axis=0)[None], (R // 8, 8, B)
        ).reshape(R, B)

    for b in range(C // B):
        cols = slice(b * B, (b + 1) * B)

        def chunk(j, state, b=b, cols=cols):
            dc, hc = state
            blk = cbuf[pl.ds(pl.multiple_of(j * R, 16), R + HP), cols]
            conv = cb_ref[:, cols]
            for k in range(K):
                o = HP - H + S * k
                conv = conv + blk[o : o + R] * taps_ref[k : k + 1, cols]
            cv = conv.astype(jnp.bfloat16)
            rg = jax.nn.sigmoid(
                jnp.dot(cv, rw_ref[b], preferred_element_type=jnp.float32) + rb_ref[:, cols])
            ig = jax.nn.sigmoid(
                jnp.dot(cv, iw_ref[b], preferred_element_type=jnp.float32) + ib_ref[:, cols])
            ld = -gate_power * rg * fr_ref[:, cols]
            a = jnp.exp(ld)
            v = jnp.sqrt(-jnp.tanh(ld) * (a * a + 1.0)) * (ig * cv.astype(jnp.float32))
            d = S
            while d < R:
                a_s = jnp.concatenate([jnp.ones((d, B), jnp.float32), a[: R - d]], axis=0)
                v_s = jnp.concatenate([jnp.zeros((d, B), jnp.float32), v[: R - d]], axis=0)
                v = a * v_s + v
                a = a * a_s
                d *= 2
            v = v + a * spreadrows(hc)
            a = a * spreadrows(dc)
            hbuf[j, :, cols] = v
            dbuf[j, :, cols] = a
            return a[R - S :], v[R - S :]

        dc, hc = lax.fori_loop(
            0, TP, chunk, (jnp.ones((S, B), jnp.float32), jnp.zeros((S, B), jnp.float32)))
        carry[sp, 0, :, cols] = dc
        carry[sp, 1, :, cols] = hc

    def carry_copy(k):
        return pltpu.make_async_remote_copy(
            carry.at[sp], carry.at[sp], c_send.at[k], c_recv.at[sp],
            device_id={"sp": (sp + k) % SP}, device_id_type=MESH)

    for k in range(1, SP):
        go(sp >= 0, functools.partial(carry_copy, k))
    if Z > 1:
        along_z(Z - 1, w_copy, lambda zz: zz, w_arrived, x_spread)
    for k in range(1, SP):
        other = (sp + k) % SP
        received(carry.at[other], c_recv.at[other])
    entering = jnp.zeros((S, C), jnp.float32)
    for k in range(SP - 1):
        entering = jnp.where(k < sp, carry[k, 0] * entering + carry[k, 1], entering)

    rows = jnp.broadcast_to(
        jnp.concatenate([entering] * (8 // S), axis=0)[None], (R // 8, 8, C)
    ).reshape(R, C)

    def gate(j):
        h = hbuf[j] + dbuf[j] * rows
        g = logits[j].astype(jnp.float32)
        gated = (h * (g / (1.0 + jnp.exp(-g)))).astype(jnp.bfloat16)
        return jnp.dot(to_seq, gated, preferred_element_type=jnp.float32).astype(jnp.bfloat16)

    def a_copy(k, e):
        target = (z + k) % Z
        row = (y + e) % Y
        return pltpu.make_async_remote_copy(
            gbuf.at[target * Y + row], ga.at[z, row], a_send.at[k, e], a_recv.at[z, e],
            device_id={"tp": target * Y + y}, device_id_type=MESH)

    for e in [*range(1, Y), 0]:
        for k in range(1, Z):
            j = (z + k) % Z * Y + (y + e) % Y
            gbuf[j] = gate(j)
            go(z >= 0, functools.partial(a_copy, k, e))
    for yy in range(Y):
        ga[z, yy] = gate(z * Y + yy)

    for k in range(1, Z):
        i = (z + k) % Z
        for d in range(1, X):
            for step in (1, -1):
                xx = x - step * d
                valid = inside(xx, X)
                q = xx * CORES + c

                @pl.when(valid)
                def _(i=i, q=q):
                    received(wf.at[i, q], w_recv.at[i, q])

                go(
                    valid & inside(x + step, X),
                    functools.partial(x_copy, i, xx, step, 0 if step == 1 else 1),
                )
                go(valid, functools.partial(core_copy, i, xx))
    for k in range(1, Z):
        i = (z + k) % Z
        for xx in range(X):
            q = xx * CORES + 1 - c
            received(wf.at[i, q], w_recv.at[i, q])

    def gated_arrived(e):
        for k in range(1, Z):
            other = (z + k) % Z
            received(ga.at[other, (y + e) % Y], a_recv.at[other, e])

    for e in range(1, Y):
        gated_arrived(e)

    tile = pbuf.shape[3]
    tiles = D // tile

    def line_sum(yy, n):
        at = slice(n * tile, (n + 1) * tile)
        acc = jnp.zeros((R, tile), jnp.float32)
        for i in range(Z):
            acc = acc + jnp.dot(
                ga[i, yy], wf[i, :, :, at].reshape(C, tile), preferred_element_type=jnp.float32)
        return acc

    def p_copy(k, n):
        return pltpu.make_async_remote_copy(
            pbuf.at[k, n], rbuf.at[k, n], p_send.at[k, n], p_recv.at[k, n],
            device_id={"tp": z * Y + (y + k) % Y}, device_id_type=MESH)

    for n in range(tiles):
        for k in range(1, Y):
            pbuf[k, n] = line_sum((y + k) % Y, n).astype(jnp.bfloat16)
            go(z >= 0, functools.partial(p_copy, k, n))
    gated_arrived(0)
    own = [line_sum(y, n) for n in range(tiles)]
    for n in range(tiles):
        total = own[n]
        for k in range(1, Y):
            received(rbuf.at[k, n], p_recv.at[k, n])
            total = total + rbuf[k, n].astype(jnp.float32)
        out_ref[:, :, n * tile : (n + 1) * tile] = total.astype(jnp.bfloat16).reshape(S, T, tile)

    for pred, make in pending:

        @pl.when(pred)
        def _(make=make):
            make().wait_send()


def per_device(
    SP, TP, Y,
    tokens, norm_gain, entry_projection, valve_projection, filter_taps, conv_bias,
    recur_weight, recur_bias, entry_weight, entry_bias, forget_rate, output_weight,
):
    S, T, D = tokens.shape
    R = S * T
    C = entry_projection.shape[1]
    HP = 16
    vmem = pl.BlockSpec(memory_space=pltpu.VMEM)
    hbm = pl.BlockSpec(memory_space=pl.ANY)
    f32, bf16 = jnp.float32, jnp.bfloat16
    dma = pltpu.SemaphoreType.DMA
    X, Z = SP // CORES, TP // Y
    tile = 512 if D % 512 == 0 else D
    return pl.pallas_call(
        functools.partial(kernel, SP, TP, Y),
        out_shape=jax.ShapeDtypeStruct(tokens.shape, bf16),
        in_specs=[vmem, vmem, hbm, hbm] + [vmem] * 7 + [hbm],
        out_specs=vmem,
        scratch_shapes=[
            pltpu.VMEM((TP, R, D), bf16),
            pltpu.VMEM((Z, SP, C // SP, D), bf16),
            pltpu.VMEM((D, C), bf16),
            pltpu.VMEM((D, C), bf16),
            pltpu.VMEM((TP * R + HP, C), f32),
            pltpu.VMEM((TP, R, C), bf16),
            pltpu.VMEM((TP, R, C), f32),
            pltpu.VMEM((TP, R, C), f32),
            pltpu.VMEM((TP, R, C), bf16),
            pltpu.VMEM((Z, Y, R, C), bf16),
            pltpu.VMEM((HP, C), f32),
            pltpu.VMEM((SP, 2, S, C), f32),
            dma((TP, 4)), dma((TP,)),
            dma((Z, 2)), dma((Z, X, 2)), dma((Z, X)), dma((Z, SP)),
            dma((Z, Y)), dma((Z, Y)), dma((SP,)), dma((SP,)),
            dma, dma, dma((Y, D // tile)), dma((Y, D // tile)), dma((2 + SP,)),
            pltpu.VMEM((Y, D // tile, R, tile), bf16),
            pltpu.VMEM((Y, D // tile, R, tile), bf16),
        ],
        compiler_params=pltpu.CompilerParams(
            collective_id=0, has_side_effects=True, vmem_limit_bytes=60 * 1024 * 1024
        ),
    )(
        tokens, norm_gain[None], entry_projection, valve_projection, filter_taps, conv_bias[None],
        recur_weight, recur_bias[None], entry_weight, entry_bias[None], forget_rate[None],
        output_weight,
    )


def solution(mesh):
    SP, TP = mesh.shape["sp"], mesh.shape["tp"]
    try:
        Y = len({tuple(d.coords)[1] for d in mesh.devices.flat})
    except AttributeError:
        Y = 1
    return jax.shard_map(
        functools.partial(per_device, SP, TP, Y),
        mesh=mesh,
        in_specs=(
            P(None, ("sp", "tp"), None),
            P(),
            P(None, "tp"),
            P(None, "tp"),
            P(None, "tp"),
            P("tp"),
            P("tp", None, None),
            P("tp"),
            P("tp", None, None),
            P("tp"),
            P("tp"),
            P("tp", None),
        ),
        out_specs=P(None, ("sp", "tp"), None),
        check_vma=False,
    )
```
